32 devices in a mesh: sp: 8 (over z, x), tp: 4 (over y, core).
Axes of the slice: x: 2, y: 2, z: 4, core: 2. Of those that a mesh axis runs over, the one named last changes fastest.
Arguments:
- latent: bfloat16 [6144, 2048], P(('sp', 'tp')), may hold values from -6 to 6
- context: bfloat16 [1024, 2048], P('sp'), may hold values from -6 to 6
- conditioning: float32 [2, 2048], replicated, may hold values from -6 to 6
- norm_gain: float32 [2048], replicated, may hold values from 0.1 to 1.9
- mod_shift: bfloat16 [2048, 2048], P('sp', 'tp'), may hold values from -0.1875 to 0.1875
- mod_scale: bfloat16 [2048, 2048], P('sp', 'tp'), may hold values from -0.1875 to 0.1875
- mod_gate: bfloat16 [2048, 2048], P('sp', 'tp'), may hold values from -0.1875 to 0.1875
- w_query: bfloat16 [2048, 2048], P(None, 'tp'), may hold values from -4 to 4
- w_key: bfloat16 [2048, 2048], P(None, 'tp'), may hold values from -0.125 to 0.125
- w_value: bfloat16 [2048, 2048], P(None, 'tp'), may hold values from -0.125 to 0.125
- w_out: bfloat16 [2048, 2048], P('tp'), may hold values from -0.125 to 0.125
- lambdas: float32 [16], P('tp'), may hold values from 0.3 to 0.8
- context_bias: float32 [16], P('tp'), may hold values from 0.8 to 2.2
- head_gain: float32 [128], replicated, may hold values from 0.1 to 1.9
Outputs:
- updated: bfloat16 [6144, 2048], P(('sp', 'tp'))
The draws below stay inside these ranges and needn't reach their ends.
All inputs are finite; a program needn't handle non-finite values.
Results may differ from the reference program's by a relative error of at most 0.01.
The reference program's roundings to bfloat16 on the way count: a program that leaves them out, or rounds other values in their place, can miss the bound.
Values may be sent and summed in bfloat16 or wider, within the bound.
A program may use at most 128 MiB of HBM per device.

```python
import math
import jax
import jax.numpy as jnp
from jax import lax

D = 2048
HEADS = 16
HD = 64
CTX = 1024
TOKENS = 6144
N_TP = 4


def draw_w_query(key, part):
    entries = jnp.clip(jax.random.normal(key, (D, HEADS * 2 * HD), jnp.float32), -6.0, 6.0) * D ** (-0.5)
    return jnp.clip(entries, -4.0, 4.0).astype(jnp.bfloat16)


def steps_of(stream_key, extent, cuts, low, high):
    def one(axis_at, shards_of):
        heights = jax.random.uniform(jax.random.fold_in(jax.random.fold_in(stream_key, 6), axis_at), (shards_of,), jnp.float32, low / len(cuts), high / len(cuts))
        return jnp.repeat(jnp.exp(heights), extent[axis_at] // shards_of).reshape((-1,) + (1,) * (len(extent) - axis_at - 1))

    loudness = one(*cuts[0])
    for cut in cuts[1:]:
        loudness = loudness * one(*cut)
    return loudness


def noise(rng, shape, spread, bound, split=(), kind=jnp.bfloat16):
    loudness = steps_of(rng, shape, split, -0.22, 0.18) if split else 1.0
    values = jax.random.normal(rng, shape, jnp.float32) * spread * loudness
    return jnp.minimum(jnp.maximum(values, -bound), bound).astype(kind)


def setup_inputs(seed: int = 0) -> dict:
    key_list = jax.random.split(jax.random.key(seed), 15)
    latent = noise(key_list[0], (TOKENS, D), 1.0, 6.0, ((0, 32),))
    context = noise(key_list[1], (CTX, D), 1.0, 6.0, ((0, 8),))
    conditioning = noise(key_list[2], (2, D), 1.0, 6.0, (), jnp.float32)
    norm_gain = jnp.clip(1.0 + 0.18 * jax.random.normal(key_list[3], (D,), jnp.float32), 0.1, 1.9)
    mod_shift = noise(key_list[4], (D, D), (D // 2) ** -0.5, 0.1875, ((0, 8), (1, 4)))
    mod_scale = noise(key_list[5], (D, D), (D // 2) ** -0.5, 0.1875, ((0, 8), (1, 4)))
    mod_gate = noise(key_list[6], (D, D), (D // 2) ** -0.5, 0.1875, ((0, 8), (1, 4)))
    w_query = draw_w_query(jax.random.fold_in(key_list[14], 71), 0)
    w_key = noise(key_list[8], (D, HEADS * 2 * HD), D ** -0.5, 0.125, ((1, 4),))
    w_value = noise(key_list[9], (D, HEADS * 2 * HD), D ** -0.5, 0.125, ((1, 4),))
    w_out = noise(key_list[10], (HEADS * 2 * HD, D), (HEADS * 2 * HD) ** -0.5, 0.125, ((0, 4),))
    lambdas = jnp.clip(0.3 + 0.5 * jax.random.uniform(key_list[11], (HEADS,), jnp.float32) ** steps_of(key_list[11], (HEADS,), ((0, 4),), -0.2, 0.2), 0.3, 0.8)
    context_bias = jnp.clip(0.8 + 1.40000004 * jax.random.uniform(key_list[12], (HEADS,), jnp.float32) ** steps_of(key_list[12], (HEADS,), ((0, 4),), -0.2, 0.2), 0.8, 2.2)
    head_gain = jnp.clip(1.0 + 0.18 * jax.random.normal(key_list[13], (2 * HD,), jnp.float32), 0.1, 1.9)
    return dict(latent=latent, context=context, conditioning=conditioning, norm_gain=norm_gain, mod_shift=mod_shift, mod_scale=mod_scale, mod_gate=mod_gate, w_query=w_query, w_key=w_key, w_value=w_value, w_out=w_out, lambdas=lambdas, context_bias=context_bias, head_gain=head_gain)


EPS = 1e-06

def modulated(inputs, norm_scale, offset_vec, scale_vec):
    rows_float = inputs.astype(jnp.float32)
    normal = rows_float * lax.rsqrt(lax.optimization_barrier(jnp.mean(rows_float * rows_float, axis=-1, keepdims=True)) + EPS)
    return (normal * norm_scale * (1.0 + scale_vec) + offset_vec).astype(jnp.bfloat16)

def reference(latent, context, conditioning, norm_gain, mod_shift, mod_scale, mod_gate, w_query, w_key, w_value, w_out, lambdas, context_bias, head_gain):
    activated = jax.nn.silu(conditioning).astype(jnp.bfloat16)
    shifts = jnp.dot(activated, mod_shift, preferred_element_type=jnp.float32)
    scales = jnp.dot(activated, mod_scale, preferred_element_type=jnp.float32)
    gates = jnp.dot(activated, mod_gate, preferred_element_type=jnp.float32)
    hidden = modulated(latent, norm_gain, shifts[0], scales[0])
    hidden_context = modulated(context, norm_gain, shifts[1], scales[1])
    latent_len = latent.shape[0]
    context_len = context.shape[0]
    keys_len = latent_len + context_len
    queries = jnp.dot(hidden, w_query, preferred_element_type=jnp.float32).astype(jnp.bfloat16).reshape(latent_len, HEADS, 2, HD)
    both_rows = jnp.concatenate([hidden_context, hidden], axis=0)
    keys = jnp.dot(both_rows, w_key, preferred_element_type=jnp.float32).astype(jnp.bfloat16).reshape(keys_len, HEADS, 2, HD)
    values = jnp.dot(both_rows, w_value, preferred_element_type=jnp.float32).astype(jnp.bfloat16).reshape(keys_len, HEADS, 2 * HD)
    context_flags = (jnp.arange(keys_len, dtype=jnp.int32) < context_len).astype(jnp.float32)
    block_len = math.gcd(latent_len, 512)

    def per_head(operands):
        query_head, key_head, value_head, lambda_head, bias_head = operands
        biases = bias_head * context_flags
        key_float = key_head.astype(jnp.float32)

        def per_block(query_block):
            query_float = query_block.astype(jnp.float32)
            per_map = []
            for which_map in range(2):
                scores = jnp.einsum('qd,kd->qk', query_float[:, which_map], key_float[:, which_map]) * HD ** (-0.5) + biases[None, :]
                peak = lax.optimization_barrier(jnp.max(scores, axis=1, keepdims=True))
                raised = jnp.exp(scores - peak)
                totals = lax.optimization_barrier(jnp.sum(raised, axis=1, keepdims=True))
                weighted = jnp.dot(raised.astype(jnp.bfloat16), value_head, preferred_element_type=jnp.float32)
                per_map.append(weighted / totals)
            return per_map[0] - lambda_head * per_map[1]
        blocks = query_head.reshape(latent_len // block_len, block_len, 2, HD)
        return lax.map(per_block, blocks).reshape(latent_len, 2 * HD)
    mixed = lax.map(per_head, (jnp.moveaxis(queries, 1, 0), jnp.moveaxis(keys, 1, 0), jnp.moveaxis(values, 1, 0), lambdas, context_bias))
    normed = mixed * lax.rsqrt(lax.optimization_barrier(jnp.mean(mixed * mixed, axis=-1, keepdims=True)) + EPS) * head_gain
    flattened = jnp.moveaxis(normed, 0, 1).reshape(latent_len, HEADS * 2 * HD).astype(jnp.bfloat16)
    group_cols = HEADS * 2 * HD // N_TP
    summed = jnp.zeros((latent_len, w_out.shape[1]), jnp.float32)
    for group_index in range(N_TP):
        lower = group_index * group_cols
        partial_value = jnp.dot(flattened[:, lower:lower + group_cols], w_out[lower:lower + group_cols], preferred_element_type=jnp.float32).astype(jnp.bfloat16)
        partial_value = lax.optimization_barrier(partial_value)
        summed = summed + partial_value.astype(jnp.float32)
    attended = summed.astype(jnp.bfloat16)
    return (latent.astype(jnp.float32) + gates[0] * attended.astype(jnp.float32)).astype(jnp.bfloat16)
```

```python
import functools, math
import jax, jax.numpy as jnp
from jax import lax
from jax.sharding import PartitionSpec as P
from jax.experimental import pallas as pl
from jax.experimental.pallas import tpu as pltpu
EPS=1e-6
LOG2E=math.log2(math.e)

def attn_kernel(cfg, lam_ref, bias_ref, q_ref, kv_ref, gain_ref, o_ref, vt_ref, m_s, l_s, a_s):
    blocks, rows, ctx, hd = cfg
    i = pl.program_id(1)
    c = hd ** -0.5 * LOG2E
    @pl.when(i == 0)
    def _():
        def tr(b, _):
            vt_ref[b] = kv_ref[b, 1].T
            return 0
        lax.fori_loop(0, blocks, tr, 0)
    q = q_ref[0]
    lane = lax.broadcasted_iota(jnp.int32, q.shape, 1)
    zero = jnp.zeros_like(q)
    qs = (jnp.where(lane < hd, q, zero), jnp.where(lane < hd, zero, q))
    m_s[...] = jnp.full_like(m_s, -1e30)
    l_s[...] = jnp.zeros_like(l_s)
    a_s[...] = jnp.zeros_like(a_s)
    bias = bias_ref[0, 0] * LOG2E
    def body(b, _):
        k = kv_ref[b, 0]
        vt = vt_ref[b]
        for m in range(2):
            s = lax.dot_general(k, qs[m], (((1,), (1,)), ((), ())), preferred_element_type=jnp.float32) * c
            s = jnp.concatenate([s[:ctx] + bias, s[ctx:]], axis=0)
            old = m_s[m]
            new = jnp.maximum(old, jnp.max(s, axis=0, keepdims=True))
            fade = jnp.exp2(old - new)
            p = jnp.exp2(s - new)
            l_s[m] = l_s[m] * fade + jnp.sum(p, axis=0, keepdims=True)
            a_s[m] = a_s[m] * fade + jnp.dot(vt, p.astype(jnp.bfloat16), preferred_element_type=jnp.float32)
            m_s[m] = new
        return 0
    lax.fori_loop(0, blocks, body, 0)
    mixed = a_s[0] / l_s[0] - lam_ref[0, 0] * (a_s[1] / l_s[1])
    normed = mixed * lax.rsqrt(jnp.mean(mixed * mixed, axis=0, keepdims=True) + EPS)
    o_ref[0] = (normed.T * gain_ref[...]).astype(jnp.bfloat16)

def attn(q, kv, ctx, lam, bias, gain, bq=256):
    heads, T, w = q.shape
    B, _, R, _ = kv.shape
    return pl.pallas_call(
        functools.partial(attn_kernel, (B, R, ctx, w // 2)),
        grid=(1, T // bq),
        in_specs=[pl.BlockSpec(memory_space=pltpu.SMEM), pl.BlockSpec(memory_space=pltpu.SMEM),
                  pl.BlockSpec((1, bq, w), lambda h, i: (h, i, 0)),
                  pl.BlockSpec((B, 2, R, w), lambda h, i: (0, 0, 0, 0)),
                  pl.BlockSpec((1, w), lambda h, i: (0, 0))],
        out_specs=pl.BlockSpec((1, bq, w), lambda h, i: (h, i, 0)),
        out_shape=jax.ShapeDtypeStruct((heads, T, w), jnp.bfloat16),
        scratch_shapes=[pltpu.VMEM((B, w, R), jnp.bfloat16), pltpu.VMEM((2, 1, bq), jnp.float32),
                        pltpu.VMEM((2, 1, bq), jnp.float32), pltpu.VMEM((2, w, bq), jnp.float32)],
    )(lam, bias, q, kv, gain)


def modulated(inputs, norm_scale, offset_vec, scale_vec):
    rows_float = inputs.astype(jnp.float32)
    normal = rows_float * lax.rsqrt(jnp.mean(rows_float * rows_float, axis=-1, keepdims=True) + EPS)
    return (normal * norm_scale * (1.0 + scale_vec) + offset_vec).astype(jnp.bfloat16)


def per_device(sizes, latent, context, conditioning, norm_gain, mod_shift, mod_scale, mod_gate, w_query, w_key, w_value, w_out, lambdas, context_bias, head_gain):
    n_sp, n_tp = sizes
    width = head_gain.shape[0]
    heads = lambdas.shape[0]
    split = math.gcd(heads, n_sp)
    rest = n_sp // split
    own = heads // split
    exchange = [[z * rest + x for z in range(split)] for x in range(rest)]
    gather = [[z * rest + x for x in range(rest)] for z in range(split)]
    place = lax.axis_index("sp")

    every_row = lax.all_gather(latent, "tp", axis=0, tiled=True)
    rows_sp = mod_shift.shape[0]
    cond_rows = lax.dynamic_slice_in_dim(conditioning, place * rows_sp, rows_sp, 1)
    activated = jax.nn.silu(cond_rows).astype(jnp.bfloat16)
    partials = jnp.stack(
        [jnp.dot(activated, matrix, preferred_element_type=jnp.float32) for matrix in (mod_shift, mod_scale, mod_gate)],
        axis=1,
    )
    parts = lax.all_gather(partials, ("sp", "tp"), axis=0, tiled=False)
    parts = parts.reshape((n_sp, n_tp) + partials.shape).sum(axis=0)
    modulation = jnp.moveaxis(parts, 0, 2).reshape(2, 3, -1)

    context_rows = modulated(context, norm_gain, modulation[1, 0], modulation[1, 1])
    rows = modulated(every_row, norm_gain, modulation[0, 0], modulation[0, 1])
    key_value = jnp.concatenate([w_key, w_value], axis=1)
    dot = functools.partial(jnp.dot, preferred_element_type=jnp.float32)
    tokens, ctx = rows.shape[0], context_rows.shape[0]
    both = jnp.concatenate([context_rows, rows], axis=0)
    count = tokens + ctx

    def by_head(matrix, columns):
        product = dot(matrix, columns).astype(jnp.bfloat16)
        return jnp.moveaxis(product.reshape(matrix.shape[0], heads, width), 1, 0)

    payload = jnp.concatenate([by_head(rows, w_query), by_head(both, w_key), by_head(both, w_value)], axis=1)
    got = lax.all_to_all(payload, "sp", 0, 0, axis_index_groups=exchange, tiled=True)
    got = got.reshape(split, own, tokens + 2 * count, width)
    queries = jnp.moveaxis(got[:, :, :tokens], 1, 0).reshape(own, split * tokens, width)
    kv = got[:, :, tokens:].reshape(split, own, 2, count, width)
    if rest > 1:
        kv = lax.all_gather(kv, "sp", axis=0, axis_index_groups=gather, tiled=True)
    start = (place // rest) * own
    lams = lax.dynamic_slice_in_dim(lambdas, start, own).reshape(own, 1)
    biases = lax.dynamic_slice_in_dim(context_bias, start, own).reshape(own, 1)
    block = max(b for b in range(8, 1025, 8) if split * tokens % b == 0)
    outs = [
        attn(queries[h : h + 1], kv[:, h], ctx, lams[h : h + 1], biases[h : h + 1], head_gain.reshape(1, width), block)
        for h in range(own)
    ]
    normed = jnp.concatenate(outs, axis=0).reshape(own, split, tokens, width)
    back = lax.all_to_all(jnp.moveaxis(normed, 1, 0), "sp", 0, 0, axis_index_groups=exchange, tiled=True)
    flattened = jnp.moveaxis(back.reshape(heads, tokens, width), 0, 1).reshape(tokens, heads * width)
    attended = lax.psum_scatter(dot(flattened, w_out).astype(jnp.bfloat16), "tp", scatter_dimension=0, tiled=True)
    return (latent.astype(jnp.float32) + modulation[0, 2] * attended.astype(jnp.float32)).astype(jnp.bfloat16)


def solution(mesh):
    sizes = (mesh.shape["sp"], mesh.shape["tp"])
    return jax.shard_map(
        functools.partial(per_device, sizes),
        mesh=mesh,
        in_specs=(P(("sp", "tp"), None), P("sp", None), P(), P(), P("sp", "tp"), P("sp", "tp"), P("sp", "tp"),
                  P(None, "tp"), P(None, "tp"), P(None, "tp"), P("tp", None), P("tp"), P("tp"), P()),
        out_specs=P(("sp", "tp"), None),
        check_vma=False,
    )
```

```python
import functools
import math
import jax
import jax.numpy as jnp
from jax import lax
from jax.experimental import pallas as pl
from jax.experimental.pallas import tpu as pltpu
from jax.sharding import PartitionSpec as P

EPS = 1e-6
LOG2E = math.log2(math.e)


def attn_kernel(cfg, lam_ref, bias_ref, q_ref, k_ref, v_ref, gain_ref, o_ref, vt_ref, m_s, l_s, a_s):
    blocks, rows, ctx, hd = cfg
    h, i = pl.program_id(0), pl.program_id(1)
    c = hd**-0.5 * LOG2E

    @pl.when(i == 0)
    def _():
        def turn(b, _):
            vt_ref[b] = v_ref[b].T
            return 0

        lax.fori_loop(0, blocks, turn, 0)

    q = q_ref[...]
    lane = lax.broadcasted_iota(jnp.int32, q.shape, 1)
    zero = jnp.zeros_like(q)
    qs = (jnp.where(lane < hd, q, zero), jnp.where(lane < hd, zero, q))
    m_s[...] = jnp.full_like(m_s, -1e30)
    l_s[...] = jnp.zeros_like(l_s)
    a_s[...] = jnp.zeros_like(a_s)
    bias = bias_ref[h] * LOG2E

    def body(b, _):
        k = k_ref[b]
        vt = vt_ref[b]
        for m in range(2):
            s = lax.dot_general(k, qs[m], (((1,), (1,)), ((), ())), preferred_element_type=jnp.float32) * c
            s = jnp.concatenate([s[:ctx] + bias, s[ctx:]], axis=0)
            old = m_s[m]
            new = jnp.maximum(old, jnp.max(s, axis=0, keepdims=True))
            fade = jnp.exp2(old - new)
            p = jnp.exp2(s - new)
            l_s[m] = l_s[m] * fade + jnp.sum(p, axis=0, keepdims=True)
            a_s[m] = a_s[m] * fade + jnp.dot(vt, p.astype(jnp.bfloat16), preferred_element_type=jnp.float32)
            m_s[m] = new
        return 0

    lax.fori_loop(0, blocks, body, 0)
    mixed = a_s[0] / l_s[0] - lam_ref[h] * (a_s[1] / l_s[1])
    normed = mixed * lax.rsqrt(jnp.mean(mixed * mixed, axis=0, keepdims=True) + EPS)
    o_ref[...] = (normed.T * gain_ref[...]).astype(jnp.bfloat16)


def attn(q, k, v, ctx, lam, bias, gain, bq):
    T, columns = q.shape
    w = gain.shape[1]
    heads = columns // w
    B, R, _ = k.shape
    ops = 8 * T * B * R * w * heads
    return pl.pallas_call(
        functools.partial(attn_kernel, (B, R, ctx, w // 2)),
        grid=(heads, T // bq),
        in_specs=[
            pl.BlockSpec(memory_space=pltpu.SMEM),
            pl.BlockSpec(memory_space=pltpu.SMEM),
            pl.BlockSpec((bq, w), lambda h, i: (i, h)),
            pl.BlockSpec((B, R, w), lambda h, i: (0, 0, h)),
            pl.BlockSpec((B, R, w), lambda h, i: (0, 0, h)),
            pl.BlockSpec((1, w), lambda h, i: (0, 0)),
        ],
        out_specs=pl.BlockSpec((bq, w), lambda h, i: (i, h)),
        out_shape=jax.ShapeDtypeStruct((T, columns), jnp.bfloat16),
        scratch_shapes=[
            pltpu.VMEM((B, w, R), jnp.bfloat16),
            pltpu.VMEM((2, 1, bq), jnp.float32),
            pltpu.VMEM((2, 1, bq), jnp.float32),
            pltpu.VMEM((2, w, bq), jnp.float32),
        ],
        cost_estimate=pl.CostEstimate(flops=4 * ops, bytes_accessed=2 * T * columns, transcendentals=2 * T * B * R * heads),
    )(lam, bias, q, k, v, gain)


def greet(peers):
    barrier = pltpu.get_barrier_semaphore()
    for peer in peers:
        pl.semaphore_signal(barrier, inc=1, device_id=peer, device_id_type=pl.DeviceIdType.MESH)
    pl.semaphore_wait(barrier, len(peers))


def remote(source, target, send, recv, peer):
    return pltpu.make_async_remote_copy(
        src_ref=source, dst_ref=target, send_sem=send, recv_sem=recv, device_id=peer, device_id_type=pl.DeviceIdType.MESH
    )


def exchange_kernel(split, rest, wide, q_ref, k_ref, v_ref, qo, ko, vo, zs, zr, xs, xr, ls):
    place = lax.axis_index("sp")
    z, x = place // rest, lax.rem(place, rest)
    z_peer = [lax.rem(z + d, split) for d in range(split)]
    x_peer = [lax.rem(x + d, rest) for d in range(rest)]
    greet([{"sp": z_peer[d] * rest + x} for d in range(1, split)] + [{"sp": z * rest + x_peer[d]} for d in range(1, rest)])

    def cols(index):
        return pl.ds(pl.multiple_of(index * wide, wide), wide)

    sends, lands = [], []
    pairs = ((k_ref, ko), (v_ref, vo))
    for d in range(1, rest):
        for a, (src, out) in enumerate(pairs):
            sends.append(remote(src.at[:, cols(z)], out.at[place], xs.at[0, d, a], xr.at[0, d, a], {"sp": z * rest + x_peer[d]}))
            sends[-1].start()
    first = {}
    for a, (src, out) in enumerate(pairs + ((q_ref, qo),)):
        for d in range(1, split):
            mine = out.at[place] if a < 2 else out.at[z]
            first[d, a] = remote(src.at[:, cols(z_peer[d])], mine, zs.at[d, a], zr.at[d, a], {"sp": z_peer[d] * rest + x})
            first[d, a].start()
    local = []
    for a, (src, out) in enumerate(pairs + ((q_ref, qo),)):
        mine = out.at[place] if a < 2 else out.at[z]
        local.append(pltpu.make_async_copy(src.at[:, cols(z)], mine, ls.at[a]))
        local[-1].start()
    for a, (src, out) in enumerate(pairs):
        for d in range(1, split):
            first[d, a].wait_recv()
            slot = lax.rem(z + split - d, split) * rest + x
            for e in range(1, rest):
                sends.append(remote(out.at[slot], out.at[slot], xs.at[d, e, a], xr.at[d, e, a], {"sp": z * rest + x_peer[e]}))
                sends[-1].start()
    for copy in local:
        copy.wait()
    for d in range(1, split):
        first[d, 2].wait_recv()
        for a in range(3):
            first[d, a].wait_send()
    for copy in sends:
        copy.wait()


def exchange(q, k, v, split, rest, wide):
    tokens, count = q.shape[0], k.shape[0]
    dma = pltpu.SemaphoreType.DMA
    vm = pl.BlockSpec(memory_space=pltpu.VMEM)
    return pl.pallas_call(
        functools.partial(exchange_kernel, split, rest, wide),
        in_specs=[vm] * 3,
        out_specs=[vm] * 3,
        out_shape=[
            jax.ShapeDtypeStruct((split, tokens, wide), q.dtype),
            jax.ShapeDtypeStruct((split * rest, count, wide), q.dtype),
            jax.ShapeDtypeStruct((split * rest, count, wide), q.dtype),
        ],
        scratch_shapes=[dma((split, 3)), dma((split, 3)), dma((split, rest, 2)), dma((split, rest, 2)), dma((3,))],
        compiler_params=pltpu.CompilerParams(collective_id=0, has_side_effects=True, vmem_limit_bytes=40 * 2**20),
        cost_estimate=pl.CostEstimate(flops=0, bytes_accessed=80_000_000, transcendentals=0),
    )(q, k, v)


def spread_kernel(split, rest, n_tp, wide, own_rows, o_ref, out_ref, ss, rs, ls):
    place, t = lax.axis_index("sp"), lax.axis_index("tp")
    z, x = place // rest, lax.rem(place, rest)
    offsets = [(d, e) for d in range(split) for e in range(n_tp)]
    peers = {(d, e): (lax.rem(z + d, split), lax.rem(t + e, n_tp)) for d, e in offsets}
    greet([{"sp": peers[o][0] * rest + x, "tp": peers[o][1]} for o in offsets[1:]])
    mine = out_ref.at[:, pl.ds(pl.multiple_of((t * split + z) * wide, wide), wide)]
    copies = []
    for d, e in offsets:
        zp, tp = peers[d, e]
        source = o_ref.at[pl.ds(pl.multiple_of((zp * n_tp + tp) * own_rows, own_rows), own_rows), :]
        if d == 0 and e == 0:
            copies.append(pltpu.make_async_copy(source, mine, ls.at[0]))
        else:
            copies.append(remote(source, mine, ss.at[d, e], rs.at[d, e], {"sp": zp * rest + x, "tp": tp}))
        copies[-1].start()
    for copy in copies:
        copy.wait()


def spread(o, split, rest, n_tp, wide, own_rows):
    dma = pltpu.SemaphoreType.DMA
    vm = pl.BlockSpec(memory_space=pltpu.VMEM)
    return pl.pallas_call(
        functools.partial(spread_kernel, split, rest, n_tp, wide, own_rows),
        in_specs=[vm],
        out_specs=vm,
        out_shape=jax.ShapeDtypeStruct((own_rows, n_tp * split * wide), o.dtype),
        scratch_shapes=[dma((split, n_tp)), dma((split, n_tp)), dma((1,))],
        compiler_params=pltpu.CompilerParams(collective_id=1, has_side_effects=True, vmem_limit_bytes=16 * 2**20),
        cost_estimate=pl.CostEstimate(flops=0, bytes_accessed=20_000_000, transcendentals=0),
    )(o)


def modulated(inputs, norm_scale, offset_vec, scale_vec):
    rows_float = inputs.astype(jnp.float32)
    normal = rows_float * lax.rsqrt(jnp.mean(rows_float * rows_float, axis=-1, keepdims=True) + EPS)
    return (normal * norm_scale * (1.0 + scale_vec) + offset_vec).astype(jnp.bfloat16)


def per_device(sizes, latent, context, conditioning, norm_gain, mod_shift, mod_scale, mod_gate, w_query, w_key, w_value, w_out, lambdas, context_bias, head_gain):
    n_sp, n_tp = sizes
    width = head_gain.shape[0]
    heads = lambdas.shape[0]
    split = math.gcd(heads, n_sp)
    rest = n_sp // split
    own = heads // split
    place = lax.axis_index("sp")

    every_row = lax.all_gather(latent, "tp", axis=0, tiled=True)
    w_out, every_row = lax.optimization_barrier((w_out, every_row))
    w_every = lax.all_gather(w_out, "tp", axis=0, tiled=True)
    rows_sp = mod_shift.shape[0]
    cond_rows = lax.dynamic_slice_in_dim(conditioning, place * rows_sp, rows_sp, 1)
    activated = jax.nn.silu(cond_rows).astype(jnp.bfloat16)
    partials = jnp.stack(
        [jnp.dot(activated, matrix, preferred_element_type=jnp.float32) for matrix in (mod_shift, mod_scale, mod_gate)],
        axis=1,
    )
    parts = lax.all_gather(partials, "sp", axis=0, tiled=False).sum(axis=0)
    modulation = lax.all_gather(parts, "tp", axis=2, tiled=True)

    context_rows = modulated(context, norm_gain, modulation[1, 0], modulation[1, 1])
    rows = modulated(every_row, norm_gain, modulation[0, 0], modulation[0, 1])
    dot = functools.partial(jnp.dot, preferred_element_type=jnp.float32)
    tokens, ctx = rows.shape[0], context_rows.shape[0]
    both = jnp.concatenate([context_rows, rows], axis=0)
    q, k, v = [
        dot(matrix, columns).astype(jnp.bfloat16) for matrix, columns in ((rows, w_query), (both, w_key), (both, w_value))
    ]
    q, k, v = exchange(q, k, v, split, rest, own * width)
    start = (place // rest) * own
    lams = lax.dynamic_slice_in_dim(lambdas, start, own)
    biases = lax.dynamic_slice_in_dim(context_bias, start, own)
    total = split * tokens
    block = max(b for b in range(8, 1025, 8) if total % b == 0)
    normed = attn(q.reshape(total, own * width), k, v, ctx, lams, biases, head_gain.reshape(1, width), block)
    flattened = spread(normed, split, rest, n_tp, own * width, latent.shape[0])
    group = heads * width
    summed = 0.0
    for g in range(n_tp):
        partial = dot(flattened[:, g * group : (g + 1) * group], w_every[g * group : (g + 1) * group])
        summed = summed + lax.reduce_precision(partial, 8, 7)
    attended = lax.reduce_precision(summed, 8, 7)
    return (latent.astype(jnp.float32) + modulation[0, 2] * attended).astype(jnp.bfloat16)


def solution(mesh):
    sizes = (mesh.shape["sp"], mesh.shape["tp"])
    return jax.shard_map(
        functools.partial(per_device, sizes),
        mesh=mesh,
        in_specs=(P(("sp", "tp"), None), P("sp", None), P(), P(), P("sp", "tp"), P("sp", "tp"), P("sp", "tp"),
                  P(None, "tp"), P(None, "tp"), P(None, "tp"), P("tp", None), P("tp"), P("tp"), P()),
        out_specs=P(("sp", "tp"), None),
        check_vma=False,
    )
```

```python
import functools
import math
import jax
import jax.numpy as jnp
from jax import lax
from jax.experimental import pallas as pl
from jax.experimental.pallas import tpu as pltpu
from jax.sharding import PartitionSpec as P

EPS = 1e-6
LOG2E = math.log2(math.e)


def greet(peers):
    barrier = pltpu.get_barrier_semaphore()
    for peer in peers:
        pl.semaphore_signal(barrier, inc=1, device_id=peer, device_id_type=pl.DeviceIdType.MESH)
    pl.semaphore_wait(barrier, len(peers))


def remote(source, target, send, recv, peer):
    return pltpu.make_async_remote_copy(
        src_ref=source, dst_ref=target, send_sem=send, recv_sem=recv, device_id=peer, device_id_type=pl.DeviceIdType.MESH
    )


def share(source, out, n_tp, me, send, recv, local):
    n_y, y, c = n_tp // 2, me // 2, lax.rem(me, 2)
    sibling = {"tp": y * 2 + 1 - c}
    copies = []
    if source is not None:
        copies.append(pltpu.make_async_copy(source, out.at[me], local))
    else:
        source = out.at[me]
    across = []
    for e in range(1, n_y):
        across.append(remote(source, out.at[me], send.at[0, e], recv.at[0, e], {"tp": lax.rem(y + e, n_y) * 2 + c}))
    copies.append(remote(source, out.at[me], send.at[1, 0], recv.at[1, 0], sibling))
    for copy in across + copies:
        copy.start()
    later = []
    for e in range(1, n_y):
        slot = lax.rem(y + n_y - e, n_y) * 2 + c
        later.append(remote(out.at[slot], out.at[slot], send.at[1, e], recv.at[1, e], sibling))

    def forward():
        for landing, copy in zip(across, later):
            landing.wait_recv()
            copy.start()

    def finish():
        for copy in across:
            copy.wait_send()
        for copy in copies + later:
            copy.wait()

    return forward, finish


def tp_peers(n_tp, me):
    n_y, y, c = n_tp // 2, me // 2, lax.rem(me, 2)
    return [{"tp": lax.rem(y + e, n_y) * 2 + c} for e in range(1, n_y)] + [{"tp": y * 2 + 1 - c}]


def opening_kernel(n_sp, n_tp, rows_ref, part_ref, rows_out, mods_out, ls, rs, rr, ms, mr, ps, pr):
    place, me = lax.axis_index("sp"), lax.axis_index("tp")
    around = [lax.rem(place + d, n_sp) for d in range(n_sp)]
    greet([{"sp": around[d]} for d in range(1, n_sp)] + tp_peers(n_tp, me))
    mine = mods_out.at[me, place]
    copies = [remote(part_ref, mine, ps.at[d], pr.at[d], {"sp": around[d]}) for d in range(1, n_sp)]
    copies.append(pltpu.make_async_copy(part_ref, mine, ls.at[0]))
    for copy in copies:
        copy.start()
    rows_on, rows_end = share(rows_ref, rows_out, n_tp, me, rs, rr, ls.at[1])
    for copy in copies:
        copy.wait()
    mods_on, mods_end = share(None, mods_out, n_tp, me, ms, mr, None)
    rows_on()
    mods_on()
    rows_end()
    mods_end()


def opening(latent, partials, n_sp, n_tp):
    dma = pltpu.SemaphoreType.DMA
    vm = pl.BlockSpec(memory_space=pltpu.VMEM)
    pair = dma((2, n_tp // 2))
    return pl.pallas_call(
        functools.partial(opening_kernel, n_sp, n_tp),
        in_specs=[vm] * 2,
        out_specs=[vm] * 2,
        out_shape=[
            jax.ShapeDtypeStruct((n_tp,) + latent.shape, latent.dtype),
            jax.ShapeDtypeStruct((n_tp, n_sp) + partials.shape, partials.dtype),
        ],
        scratch_shapes=[dma((2,)), pair, pair, pair, pair, dma((n_sp,)), dma((n_sp,))],
        compiler_params=pltpu.CompilerParams(collective_id=2, has_side_effects=True, vmem_limit_bytes=32 * 2**20),
        cost_estimate=pl.CostEstimate(flops=0, bytes_accessed=40_000_000, transcendentals=0),
    )(latent, partials)


def attend_kernel(cfg, lam_ref, bias_ref, gain_ref, q_ref, k_ref, v_ref, w_ref, o_ref, wo, qo, ko, vo, vt_ref, m_s, l_s, a_s, zs, zr, xs, xr, ls, ws, wr):
    split, rest, n_tp, own, width, ctx = cfg
    wide = own * width
    half = width // 2
    c = half**-0.5 * LOG2E
    place, me = lax.axis_index("sp"), lax.axis_index("tp")
    z, x = place // rest, lax.rem(place, rest)
    z_peer = [lax.rem(z + d, split) for d in range(split)]
    x_peer = [{"sp": z * rest + lax.rem(x + d, rest)} for d in range(rest)]
    greet([{"sp": z_peer[d] * rest + x} for d in range(1, split)] + x_peer[1:] + tp_peers(n_tp, me))

    def cols(index):
        return pl.ds(pl.multiple_of(index * wide, wide), wide)

    pairs = ((k_ref, ko), (v_ref, vo))
    outward = []
    for a, (src, out) in enumerate(pairs):
        for e in range(1, rest):
            outward.append(remote(src.at[:, cols(z)], out.at[place], xs.at[0, e, a], xr.at[0, e, a], x_peer[e]))
    for a, (src, out) in ((2, (q_ref, qo)),) + tuple(enumerate(pairs)):
        for d in range(1, split):
            mine = out.at[place] if a < 2 else out.at[z]
            outward.append(remote(src.at[:, cols(z_peer[d])], mine, zs.at[d, a], zr.at[d, a], {"sp": z_peer[d] * rest + x}))
    local = []
    for a, (src, out) in enumerate(pairs + ((q_ref, qo),)):
        mine = out.at[place] if a < 2 else out.at[z]
        local.append(pltpu.make_async_copy(src.at[:, cols(z)], mine, ls.at[a]))
    for copy in outward + local:
        copy.start()
    w_on, w_end = share(w_ref, wo, n_tp, me, ws, wr, ls.at[3])
    m_s[...] = jnp.full_like(m_s, -1e30)
    l_s[...] = jnp.zeros_like(l_s)
    a_s[...] = jnp.zeros_like(a_s)
    for copy in local:
        copy.wait()

    def onward(slot, d, e, a, out):
        return remote(out.at[slot], out.at[slot], xs.at[d, e, a], xr.at[d, e, a], x_peer[e] if isinstance(e, int) else x_peer[-1])

    def landed(d, a, out, slot):
        return remote(out.at[slot], out.at[slot], zs.at[d, a], zr.at[d, a], x_peer[-1])

    def absorb(j, _):
        d, e = j // rest, lax.rem(j, rest)
        from_z = lax.rem(z + split - d, split)
        slot = from_z * rest + lax.rem(x + rest - e, rest)

        @pl.when((e == 0) & (d > 0))
        def _():
            for a, (_, out) in enumerate(pairs):
                landed(d, a, out, slot).wait_recv()
                for f in range(1, rest):
                    onward(slot, d, f, a, out).start()

        @pl.when(e > 0)
        def _():
            for a, (_, out) in enumerate(pairs):
                onward(slot, d, e, a, out).wait_recv()

        @pl.when(j == split * rest // 2)
        def _():
            w_on()

        for h in range(own):
            vt_ref[...] = vo[slot, :, h * width : (h + 1) * width].T
            bias = bias_ref[h] * LOG2E

            def queries(i, _):
                zq = lax.rem(z + split - i, split)
                if h == 0:

                    @pl.when((j == 0) & (i > 0))
                    def _():
                        remote(qo.at[zq], qo.at[zq], zs.at[i, 2], zr.at[i, 2], x_peer[-1]).wait_recv()

                q = qo[zq, :, h * width : (h + 1) * width]
                k = ko[slot, :, h * width : (h + 1) * width]
                vt = vt_ref[...]
                lane = lax.broadcasted_iota(jnp.int32, q.shape, 1)
                zero = jnp.zeros_like(q)
                for m, chosen in enumerate((jnp.where(lane < half, q, zero), jnp.where(lane < half, zero, q))):
                    n = h * 2 + m
                    s = lax.dot_general(k, chosen, (((1,), (1,)), ((), ())), preferred_element_type=jnp.float32) * c
                    s = jnp.concatenate([s[:ctx] + bias, s[ctx:]], axis=0)
                    old = m_s[n, zq]
                    new = jnp.maximum(old, jnp.max(s, axis=0, keepdims=True))
                    fade = jnp.exp2(old - new)
                    p = jnp.exp2(s - new)
                    l_s[n, zq] = l_s[n, zq] * fade + jnp.sum(p, axis=0, keepdims=True)
                    a_s[n, zq] = a_s[n, zq] * fade + jnp.dot(vt, p.astype(jnp.bfloat16), preferred_element_type=jnp.float32)
                    m_s[n, zq] = new
                return 0

            lax.fori_loop(0, split, queries, 0)
        return 0

    lax.fori_loop(0, split * rest, absorb, 0)

    def close(zq, _):
        for h in range(own):
            mixed = a_s[2 * h, zq] / l_s[2 * h, zq] - lam_ref[h] * (a_s[2 * h + 1, zq] / l_s[2 * h + 1, zq])
            normed = mixed * lax.rsqrt(jnp.mean(mixed * mixed, axis=0, keepdims=True) + EPS)
            o_ref[zq, :, h * width : (h + 1) * width] = (normed.T * gain_ref[...]).astype(jnp.bfloat16)
        return 0

    lax.fori_loop(0, split, close, 0)
    for copy in outward:
        copy.wait_send()
    for d in range(1, split):
        slot = lax.rem(z + split - d, split) * rest + x
        for e in range(1, rest):
            for a, (_, out) in enumerate(pairs):
                onward(slot, d, e, a, out).wait_send()
    w_end()


def attend(q, k, v, w_out, lam, bias, gain, split, rest, n_tp, own, ctx):
    tokens, count = q.shape[0], k.shape[0]
    width = gain.shape[1]
    wide = own * width
    dma = pltpu.SemaphoreType.DMA
    vm = pl.BlockSpec(memory_space=pltpu.VMEM)
    sm = pl.BlockSpec(memory_space=pltpu.SMEM)
    stat = pltpu.VMEM((2 * own, split, 1, tokens), jnp.float32)
    return pl.pallas_call(
        functools.partial(attend_kernel, (split, rest, n_tp, own, width, ctx)),
        in_specs=[sm, sm] + [vm] * 5,
        out_specs=[vm, pl.BlockSpec(memory_space=pl.ANY)],
        out_shape=[
            jax.ShapeDtypeStruct((split, tokens, wide), q.dtype),
            jax.ShapeDtypeStruct((n_tp,) + w_out.shape, w_out.dtype),
        ],
        scratch_shapes=[
            pltpu.VMEM((split, tokens, wide), q.dtype),
            pltpu.VMEM((split * rest, count, wide), q.dtype),
            pltpu.VMEM((split * rest, count, wide), q.dtype),
            pltpu.VMEM((width, count), q.dtype),
            stat,
            stat,
            pltpu.VMEM((2 * own, split, width, tokens), jnp.float32),
            dma((split, 3)),
            dma((split, 3)),
            dma((split, rest, 2)),
            dma((split, rest, 2)),
            dma((4,)),
            dma((2, n_tp // 2)),
            dma((2, n_tp // 2)),
        ],
        compiler_params=pltpu.CompilerParams(collective_id=0, has_side_effects=True, vmem_limit_bytes=56 * 2**20),
        cost_estimate=pl.CostEstimate(flops=50_000_000_000, bytes_accessed=80_000_000, transcendentals=0),
    )(lam, bias, gain, q, k, v, w_out)


def spread_kernel(split, rest, n_tp, wide, own_rows, o_ref, out_ref, ss, rs, ls):
    place, t = lax.axis_index("sp"), lax.axis_index("tp")
    z, x = place // rest, lax.rem(place, rest)
    offsets = [(d, e) for d in range(split) for e in range(n_tp)]
    peers = {(d, e): (lax.rem(z + d, split), lax.rem(t + e, n_tp)) for d, e in offsets}
    greet([{"sp": peers[o][0] * rest + x, "tp": peers[o][1]} for o in offsets[1:]])
    mine = out_ref.at[:, pl.ds(pl.multiple_of((t * split + z) * wide, wide), wide)]
    copies = []
    for d, e in offsets:
        zp, tp = peers[d, e]
        source = o_ref.at[pl.ds(pl.multiple_of((zp * n_tp + tp) * own_rows, own_rows), own_rows), :]
        if d == 0 and e == 0:
            copies.append(pltpu.make_async_copy(source, mine, ls.at[0]))
        else:
            copies.append(remote(source, mine, ss.at[d, e], rs.at[d, e], {"sp": zp * rest + x, "tp": tp}))
        copies[-1].start()
    for copy in copies:
        copy.wait()


def spread(o, split, rest, n_tp, wide, own_rows):
    dma = pltpu.SemaphoreType.DMA
    vm = pl.BlockSpec(memory_space=pltpu.VMEM)
    return pl.pallas_call(
        functools.partial(spread_kernel, split, rest, n_tp, wide, own_rows),
        in_specs=[vm],
        out_specs=vm,
        out_shape=jax.ShapeDtypeStruct((own_rows, n_tp * split * wide), o.dtype),
        scratch_shapes=[dma((split, n_tp)), dma((split, n_tp)), dma((1,))],
        compiler_params=pltpu.CompilerParams(collective_id=1, has_side_effects=True, vmem_limit_bytes=16 * 2**20),
        cost_estimate=pl.CostEstimate(flops=0, bytes_accessed=20_000_000, transcendentals=0),
    )(o)


def modulated(inputs, norm_scale, offset_vec, scale_vec):
    rows_float = inputs.astype(jnp.float32)
    normal = rows_float * lax.rsqrt(jnp.mean(rows_float * rows_float, axis=-1, keepdims=True) + EPS)
    return (normal * norm_scale * (1.0 + scale_vec) + offset_vec).astype(jnp.bfloat16)


def per_device(sizes, latent, context, conditioning, norm_gain, mod_shift, mod_scale, mod_gate, w_query, w_key, w_value, w_out, lambdas, context_bias, head_gain):
    n_sp, n_tp = sizes
    width = head_gain.shape[0]
    heads = lambdas.shape[0]
    split = math.gcd(heads, n_sp)
    rest = n_sp // split
    own = heads // split
    place = lax.axis_index("sp")

    rows_sp = mod_shift.shape[0]
    cond_rows = lax.dynamic_slice_in_dim(conditioning, place * rows_sp, rows_sp, 1)
    activated = jax.nn.silu(cond_rows).astype(jnp.bfloat16)
    products = [jnp.dot(activated, matrix, preferred_element_type=jnp.float32) for matrix in (mod_shift, mod_scale, mod_gate)]
    partials = jnp.concatenate(products + [jnp.zeros_like(products[0])], axis=0)
    every_row, parts = opening(latent, partials, n_sp, n_tp)
    every_row = every_row.reshape(n_tp * latent.shape[0], latent.shape[1])
    summed = parts.sum(axis=1)
    modulation = jnp.moveaxis(summed, 0, 1).reshape(4, 2, -1).swapaxes(0, 1)

    context_rows = modulated(context, norm_gain, modulation[1, 0], modulation[1, 1])
    rows = modulated(every_row, norm_gain, modulation[0, 0], modulation[0, 1])
    dot = functools.partial(jnp.dot, preferred_element_type=jnp.float32)
    tokens, ctx = rows.shape[0], context_rows.shape[0]
    both = jnp.concatenate([context_rows, rows], axis=0)
    q, k, v = [
        dot(matrix, columns).astype(jnp.bfloat16) for matrix, columns in ((rows, w_query), (both, w_key), (both, w_value))
    ]
    start = (place // rest) * own
    lams = lax.dynamic_slice_in_dim(lambdas, start, own)
    biases = lax.dynamic_slice_in_dim(context_bias, start, own)
    normed, w_every = attend(q, k, v, w_out, lams, biases, head_gain.reshape(1, width), split, rest, n_tp, own, ctx)
    normed = normed.reshape(split * tokens, own * width)
    flattened = spread(normed, split, rest, n_tp, own * width, latent.shape[0])
    group = heads * width
    summed = 0.0
    for g in range(n_tp):
        partial = dot(flattened[:, g * group : (g + 1) * group], w_every[g])
        summed = summed + lax.reduce_precision(partial, 8, 7)
    attended = lax.reduce_precision(summed, 8, 7)
    return (latent.astype(jnp.float32) + modulation[0, 2] * attended).astype(jnp.bfloat16)


def solution(mesh):
    sizes = (mesh.shape["sp"], mesh.shape["tp"])
    return jax.shard_map(
        functools.partial(per_device, sizes),
        mesh=mesh,
        in_specs=(P(("sp", "tp"), None), P("sp", None), P(), P(), P("sp", "tp"), P("sp", "tp"), P("sp", "tp"),
                  P(None, "tp"), P(None, "tp"), P(None, "tp"), P("tp", None), P("tp"), P("tp"), P()),
        out_specs=P(("sp", "tp"), None),
        check_vma=False,
    )
```
